32 devices in a mesh: ep: 4 (over y, x), tp: 8 (over z, core).
Axes of the slice: x: 2, y: 2, z: 4, core: 2. Of those that a mesh axis runs over, the one named last changes fastest.
Arguments:
- mix_tokens: bfloat16 [512, 4096], P('ep'), may hold values from -6 to 6
- mix_gain: float32 [4096], replicated, may hold values from 0.1 to 1.9
- value_weight: bfloat16 [4096, 2048], P(None, 'tp'), may hold values from -0.09375 to 0.09375
- inner_weight: bfloat16 [4096, 2048], P(None, 'tp'), may hold values from -0.09375 to 0.09375
- outer_weight: bfloat16 [4096, 2048], P(None, 'tp'), may hold values from -0.09375 to 0.09375
- conv_taps: float32 [3, 2048], P(None, 'tp'), may hold values from -3 to 3
- mix_weight: bfloat16 [2048, 4096], P('tp'), may hold values from -0.125 to 0.125
- moe_tokens: bfloat16 [512, 4096], P('ep'), may hold values from -6 to 6
- moe_gain: float32 [4096], replicated, may hold values from 0.1 to 1.9
- router_group: bfloat16 [4096, 4], replicated, may hold values from -0.09375 to 0.09375
- router_expert: bfloat16 [4096, 16], replicated, may hold values from -0.09375 to 0.09375
- expert_routes: int32 [512, 2], P('ep'), may hold values from 0 to 15, as said below
- gate_weight: bfloat16 [16, 4096, 2048], P('ep', None, 'tp'), may hold values from -0.09375 to 0.09375
- up_weight: bfloat16 [16, 4096, 2048], P('ep', None, 'tp'), may hold values from -0.09375 to 0.09375
- down_weight: bfloat16 [16, 2048, 4096], P('ep', 'tp'), may hold values from -0.5 to 0.5
Outputs:
- mixer_out: bfloat16 [512, 4096], P(('ep', 'tp'))
- expert_out: bfloat16 [512, 4096], P(('ep', 'tp'))
The draws below stay inside these ranges and needn't reach their ends.
Inputs may be any that keep to these rules, and one draw needn't show every extreme that they name: `expert_routes`: the two experts of a row are different and lie in one group of 4 consecutive expert numbers. In each aligned block of 16 rows no expert is named more than 4 times, and in every draw some experts are named exactly 4 times in every block.
All inputs are finite; a program needn't handle non-finite values.
Results may differ from the reference program's by a relative error of at most 0.0076.
Values may be sent and summed in bfloat16 or wider, within the bound.
A program may use at most 128 MiB of HBM per device.

```python
import jax
import jax.numpy as jnp
from jax import lax

D = 4096
CONV_CH = 2048
TAPS = 3
FE = 2048
EXPERTS = 16
GROUPS = 4
TOPK = 2
MOE_SHARE = 16
EPG = 4
CAP = 4
MIX_TOKENS = 512
MOE_TOKENS = 512


def draw_expert_routes(key, part):
    blocks = MOE_TOKENS // MOE_SHARE
    half_share = MOE_SHARE // 2
    subkeys = jax.random.split(jax.random.fold_in(key, 7), 5)
    hot_group = jax.random.randint(subkeys[0], (), 0, GROUPS).astype(jnp.int32)
    others = (hot_group + 1 + jax.random.randint(subkeys[1], (blocks, MOE_SHARE - half_share), 0, GROUPS - 1)) % GROUPS
    labels = jnp.concatenate([jnp.full((blocks, half_share), hot_group, jnp.int32), others.astype(jnp.int32)], axis=1)
    scores = jax.random.randint(subkeys[2], (blocks, MOE_SHARE), 0, 1048576) * MOE_SHARE + jnp.arange(MOE_SHARE, dtype=jnp.int32)[None, :]
    ordering = jnp.argsort(scores, axis=1, stable=True)
    labels = jnp.take_along_axis(labels, ordering, axis=1)
    one_hot = (labels[:, :, None] == jnp.arange(GROUPS, dtype=jnp.int32)[None, None, :]).astype(jnp.int32)
    within = jnp.sum((jnp.cumsum(one_hot, axis=1) - one_hot) * one_hot, axis=2)
    offsets = jax.random.randint(subkeys[3], (blocks, GROUPS), 0, EPG)
    strides = jax.random.randint(subkeys[4], (blocks, GROUPS), 1, EPG)
    offset_tok = jnp.take_along_axis(offsets, labels, axis=1)
    stride_tok = jnp.take_along_axis(strides, labels, axis=1)
    first_pick = labels * EPG + (within + offset_tok) % EPG
    second_pick = labels * EPG + (within + offset_tok + stride_tok) % EPG
    return jnp.stack([first_pick, second_pick], axis=-1).reshape(blocks * MOE_SHARE, TOPK).astype(jnp.int32)


def levels(rng, shape, cuts, smallest, top_value):
    loudness = 1.0
    for dim, shards_of in cuts:
        draws = jax.random.uniform(jax.random.fold_in(jax.random.fold_in(rng, 6), dim), (shards_of,), jnp.float32, smallest / len(cuts), top_value / len(cuts))
        loudness = loudness * jnp.repeat(jnp.exp(draws), shape[dim] // shards_of).reshape((-1,) + (1,) * (len(shape) - 1 - dim))
    return loudness


def bell_draw(own_key, dims, deviation, limit, cuts=(), kind=jnp.bfloat16):
    values = deviation * jax.random.normal(own_key, dims, jnp.float32)
    if cuts:
        values = values * levels(own_key, dims, cuts, -0.22, 0.18)
    return jnp.clip(values, -limit, limit).astype(kind)


def setup_inputs(seed: int = 0) -> dict:
    seeds = jax.random.split(jax.random.key(seed), 16)
    return {
        "mix_tokens": bell_draw(seeds[0], (MIX_TOKENS, D), 1.0, 6.0, ((0, 4),)),
        "mix_gain": jnp.clip(1.0 + 0.18 * jax.random.normal(seeds[1], (D,), jnp.float32), 0.1, 1.9),
        "value_weight": bell_draw(seeds[2], (D, CONV_CH), D ** -0.5, 0.09375, ((1, 8),)),
        "inner_weight": bell_draw(seeds[3], (D, CONV_CH), D ** -0.5, 0.09375, ((1, 8),)),
        "outer_weight": bell_draw(seeds[4], (D, CONV_CH), D ** -0.5, 0.09375, ((1, 8),)),
        "conv_taps": bell_draw(seeds[5], (TAPS, CONV_CH), 0.6, 3.0, ((1, 8),), jnp.float32),
        "mix_weight": bell_draw(seeds[6], (CONV_CH, D), CONV_CH ** -0.5, 0.125, ((0, 8),)),
        "moe_tokens": bell_draw(seeds[7], (MOE_TOKENS, D), 1.0, 6.0, ((0, 4),)),
        "moe_gain": jnp.clip(1.0 + 0.18 * jax.random.normal(seeds[8], (D,), jnp.float32), 0.1, 1.9),
        "router_group": bell_draw(seeds[9], (D, GROUPS), D ** -0.5, 0.09375),
        "router_expert": bell_draw(seeds[10], (D, EXPERTS), D ** -0.5, 0.09375),
        "expert_routes": draw_expert_routes(jax.random.fold_in(seeds[15], 71), 0),
        "gate_weight": bell_draw(seeds[12], (EXPERTS, D, FE), D ** -0.5, 0.09375, ((0, 4), (2, 8))),
        "up_weight": bell_draw(seeds[13], (EXPERTS, D, FE), D ** -0.5, 0.09375, ((0, 4), (2, 8))),
        "down_weight": bell_draw(seeds[14], (EXPERTS, FE, D), (FE // 16) ** -0.5, 0.5, ((0, 4), (1, 8))),
    }


def rms_rows(inputs, gain_vec):
    values = inputs.astype(jnp.float32)
    inverse = lax.rsqrt(lax.optimization_barrier(jnp.mean(values * values, axis=-1, keepdims=True)) + 1e-06)
    return (values * inverse * gain_vec.astype(jnp.float32)).astype(jnp.bfloat16)

def route_weights(normed, routes, router_group, router_expert):
    group_logit = jnp.dot(normed, router_group, preferred_element_type=jnp.float32)
    expert_logit = jnp.dot(normed, router_expert, preferred_element_type=jnp.float32)
    group_exp = jnp.exp(group_logit)
    group_id = routes[:, 0] // EPG
    group_pick = (group_id[:, None] == jnp.arange(GROUPS, dtype=jnp.int32)[None, :]).astype(jnp.float32)
    group_gate = lax.optimization_barrier(jnp.sum(group_exp * group_pick, axis=1)) / lax.optimization_barrier(jnp.sum(group_exp, axis=1))
    expert_pick = (routes[:, :, None] == jnp.arange(EXPERTS, dtype=jnp.int32)[None, None, :]).astype(jnp.float32)
    chosen = jnp.exp(lax.optimization_barrier(jnp.sum(expert_logit[:, None, :] * expert_pick, axis=2)))
    return group_gate[:, None] * chosen / lax.optimization_barrier(jnp.sum(chosen, axis=1, keepdims=True))

def slot_ranks(routes):
    blocks = routes.shape[0] // MOE_SHARE
    entries = routes.reshape(blocks, MOE_SHARE * TOPK)
    one_hot = (entries[:, :, None] == jnp.arange(EXPERTS, dtype=jnp.int32)[None, None, :]).astype(jnp.int32)
    before = jnp.cumsum(one_hot, axis=1) - one_hot
    return lax.optimization_barrier(jnp.sum(before * one_hot, axis=2)).reshape(routes.shape)

def reference(mix_tokens, mix_gain, value_weight, inner_weight, outer_weight, conv_taps, mix_weight, moe_tokens, moe_gain, router_group, router_expert, expert_routes, gate_weight, up_weight, down_weight):
    normed = rms_rows(mix_tokens, mix_gain)
    value_proj = jnp.dot(normed, value_weight, preferred_element_type=jnp.float32)
    inner_proj = jnp.dot(normed, inner_weight, preferred_element_type=jnp.float32)
    outer_proj = jnp.dot(normed, outer_weight, preferred_element_type=jnp.float32)
    gated_in = lax.optimization_barrier((inner_proj * value_proj).astype(jnp.bfloat16)).astype(jnp.float32)
    seq_rows = gated_in.shape[0]
    padded = jnp.concatenate([jnp.zeros((TAPS - 1, gated_in.shape[1]), jnp.float32), gated_in], axis=0)
    tap_values = conv_taps.astype(jnp.float32)
    mixed_conv = tap_values[0] * padded[0:seq_rows]
    for tap_index in range(1, TAPS):
        mixed_conv = mixed_conv + tap_values[tap_index] * padded[tap_index:tap_index + seq_rows]
    conv_out = (outer_proj * mixed_conv).astype(jnp.bfloat16)
    mixer_out = jnp.dot(conv_out, mix_weight, preferred_element_type=jnp.float32).astype(jnp.bfloat16)
    moe_normed = rms_rows(moe_tokens, moe_gain)
    weights = route_weights(moe_normed, expert_routes, router_group, router_expert)
    ranks = slot_ranks(expert_routes)
    total_rows = moe_tokens.shape[0]
    block_id = jnp.arange(total_rows, dtype=jnp.int32) // MOE_SHARE
    position = (block_id[:, None] * CAP + ranks).astype(jnp.int32)
    per_expert = total_rows // MOE_SHARE * CAP
    token_id = jnp.broadcast_to(jnp.arange(total_rows, dtype=jnp.int32)[:, None], (total_rows, TOPK))
    slot_table = jnp.zeros((EXPERTS, per_expert), jnp.int32).at[expert_routes, position].set(token_id)

    def run_expert(operands):
        row_index, gate_w, up_w, down_w = operands
        picked_rows = moe_normed[row_index]
        gate_proj = jnp.dot(picked_rows, gate_w, preferred_element_type=jnp.float32)
        up_proj = jnp.dot(picked_rows, up_w, preferred_element_type=jnp.float32)
        hidden = (jax.nn.silu(gate_proj) * up_proj).astype(jnp.bfloat16)
        summed = jnp.dot(hidden, down_w, preferred_element_type=jnp.float32)
        return summed.astype(jnp.bfloat16)
    results = lax.map(run_expert, (slot_table, gate_weight, up_weight, down_weight))
    picked = results[expert_routes, position].astype(jnp.float32)
    expert_out = lax.optimization_barrier(jnp.sum(weights[:, :, None] * picked, axis=1)).astype(jnp.bfloat16)
    return (mixer_out, expert_out)
```

```python
import functools

import jax
import jax.numpy as jnp
from jax import lax
from jax.experimental import pallas as pl
from jax.experimental.pallas import tpu as pltpu
from jax.sharding import PartitionSpec as P

EPG = 4
CAP = 4
CORES = 2
CHUNKS = 4
MESH = pl.DeviceIdType.MESH
F32, BF16 = jnp.float32, jnp.bfloat16


def iota(shape, dim):
    return lax.broadcasted_iota(jnp.int32, shape, dim)


def norm_rows(src, gain, dst):
    width = src.shape[1]

    def body(i, carry):
        rows = pl.ds(pl.multiple_of(i * 16, 16), 16)
        x = src[rows, :].astype(F32)
        inv = lax.rsqrt(jnp.sum(x * x, axis=1, keepdims=True) * (1.0 / width) + 1e-06)
        dst[rows, :] = (x * inv * gain[...]).astype(BF16)
        return carry

    lax.fori_loop(0, src.shape[0] // 16, body, 0)


def column_tiles(width, tile, body):
    def step(i, carry):
        body(pl.ds(pl.multiple_of(i * tile, tile), tile))
        return carry

    lax.fori_loop(0, width // tile, step, 0)


def kernel(
    cfg,
    mix_tokens, mix_gain, value_w, inner_w, outer_w, taps, mix_w, moe_tokens, moe_gain,
    router_group, router_expert, routes, gate_w, up_w, down_w,
    mixer_out, expert_out,
    xm, xe, rg, rx, vw, iw, ow, mw, gw, uw, dw,
    nm, ne, spread, pack, got, wpack, wgot, wrow,
    gated, halo, padded, conv, pair_out, pair_in, keep, zin,
    hid, y_out, y_in, y_keep, e_in, s_keep, s_out, s_in,
    load_sem, gate_sem, up_sem, down_sem,
    disp_s, disp_r, w_s, w_r, fwd_s, fwd_r, halo_s, halo_r, mp_s, mp_r, mz_s, mz_r,
    yp_s, yp_r, ye_s, ye_r, yz_s, yz_r,
):
    ep, tp, zs, half, experts_here = cfg
    e_me, t_me = lax.axis_index("ep"), lax.axis_index("tp")
    z_me, c_me = t_me // CORES, lax.rem(t_me, CORES)
    c_no = 1 - c_me
    partner = z_me * CORES + c_no
    width = xm.shape[1]
    ep_peers = [lax.rem(e_me + d, ep) for d in range(1, ep)]
    z_peers = [lax.rem(z_me + d, zs) for d in range(1, zs)]

    barrier = pltpu.get_barrier_semaphore()
    for e in ep_peers:
        pl.semaphore_signal(barrier, inc=1, device_id={"ep": e, "tp": t_me}, device_id_type=MESH)
    for z in z_peers:
        pl.semaphore_signal(
            barrier, inc=1, device_id={"ep": e_me, "tp": z * CORES + c_me}, device_id_type=MESH
        )
    pl.semaphore_signal(barrier, inc=1, device_id={"ep": e_me, "tp": partner}, device_id_type=MESH)

    def load(k, src, dst):
        return pltpu.make_async_copy(src, dst, load_sem.at[k])

    loads = [
        load(k, s, d)
        for k, (s, d) in enumerate(
            [
                (moe_tokens, xe), (router_group, rg), (router_expert, rx), (mix_tokens, xm),
                (value_w, vw), (inner_w, iw), (outer_w, ow), (mix_w, mw),
            ]
        )
    ]
    for c in loads:
        c.start()

    def remote(src, dst, s_sem, r_sem, e, t):
        return pltpu.make_async_remote_copy(
            src_ref=src, dst_ref=dst, send_sem=s_sem, recv_sem=r_sem,
            device_id={"ep": e, "tp": t}, device_id_type=MESH,
        )

    loads[0].wait()
    norm_rows(xe, moe_gain, ne)
    count = xe.shape[0]
    share = count // tp
    slots = half // zs
    span = ep * half
    r = routes[...]
    picks = [r[:, 0:1], r[:, 1:2]]
    lane = iota((count, 128), 1)
    shards = [
        sum((p >= s * experts_here).astype(jnp.int32) for s in range(1, ep)) for p in picks
    ]
    member = jnp.where((lane == shards[0]) | (lane == shards[1]), 1.0, 0.0).astype(BF16)
    ti, tj = iota((count, count), 0), iota((count, count), 1)
    earlier = jnp.where(((ti ^ tj) < share) & (tj < ti), 1.0, 0.0).astype(BF16)
    rank = jnp.dot(earlier, member, preferred_element_type=F32)
    block = lax.shift_right_logical(iota((count, 1), 0), share.bit_length() - 1)
    base = (block & 1) * span + lax.shift_right_logical(block, 1) * slots
    slot_lane = iota((count, 2 * span), 1)
    hits = []
    for s in shards:
        mine = jnp.sum(jnp.where(lane == s, rank, 0.0), axis=1, keepdims=True).astype(jnp.int32)
        hits.append(slot_lane == base + s * half + mine)
    one_hot = jnp.where(hits[0] | hits[1], 1.0, 0.0).astype(BF16)
    spread[...] = one_hot

    def pack_tile(cols):
        pack[:, cols] = lax.dot_general(
            spread[...], ne[:, cols], (((0,), (0,)), ((), ())), preferred_element_type=F32
        ).astype(BF16)

    column_tiles(width, 512, pack_tile)

    pl.semaphore_wait(barrier, (ep - 1) + (zs - 1) + 1)
    sends = []

    def go(copy):
        copy.start()
        sends.append(copy)

    def half_rows(c, e):
        return pl.ds(pl.multiple_of(c * span + e * half, half), half)

    for e in ep_peers:
        go(
            remote(
                pack.at[half_rows(c_me, e), :], got.at[half_rows(c_me, e_me), :],
                disp_s.at[e], disp_r.at[e_me], e, t_me,
            )
        )
    for k in range(experts_here):
        pltpu.make_async_copy(gate_w.at[k], gw.at[k], gate_sem.at[k]).start()
        pltpu.make_async_copy(up_w.at[k], uw.at[k], up_sem.at[k]).start()
    for k in range(experts_here):
        pltpu.make_async_copy(down_w.at[k], dw.at[k], down_sem.at[k]).start()

    loads[1].wait()
    loads[2].wait()
    group_exp = jnp.exp(jnp.dot(ne[...], rg[...], preferred_element_type=F32))
    expert_logit = jnp.dot(ne[...], rx[...], preferred_element_type=F32)
    groups, experts = group_exp.shape[1], expert_logit.shape[1]
    group = sum((picks[0] >= s * EPG).astype(jnp.int32) for s in range(1, groups))
    chosen_group = jnp.where(iota((count, groups), 1) == group, group_exp, 0.0)
    group_gate = jnp.sum(chosen_group, axis=1, keepdims=True) / jnp.sum(
        group_exp, axis=1, keepdims=True
    )
    expert_lane = iota((count, experts), 1)
    chosen = [
        jnp.exp(jnp.sum(jnp.where(expert_lane == p, expert_logit, 0.0), axis=1, keepdims=True))
        for p in picks
    ]
    scale = chosen[0] + chosen[1]
    weights = sum(
        jnp.where(lane == p, group_gate * c / scale, 0.0) for p, c in zip(picks, chosen)
    )
    parts, rest = [], weights
    for _ in range(3):
        parts.append(rest.astype(BF16))
        rest = rest - parts[-1].astype(F32)
    packed_w = sum(
        lax.dot_general(spread[...], p, (((0,), (0,)), ((), ())), preferred_element_type=F32)
        for p in parts
    )
    for e in range(ep):
        for c in range(CORES):
            wpack[e, c * half : (c + 1) * half, :] = packed_w[
                c * span + e * half : c * span + (e + 1) * half, :
            ]
    for e in ep_peers:
        go(remote(wpack.at[e], wgot.at[e_me], w_s.at[e], w_r.at[e_me], e, t_me))
    wgot[e_me] = wpack[e_me]
    for c in range(CORES):
        got[half_rows(c, e_me), :] = pack[half_rows(c, e_me), :]

    loads[3].wait()
    norm_rows(xm, mix_gain, nm)
    loads[4].wait()
    loads[5].wait()
    rows = xm.shape[0]
    value_proj = jnp.dot(nm[...], vw[...], preferred_element_type=F32)
    inner_proj = jnp.dot(nm[...], iw[...], preferred_element_type=F32)
    gated[...] = (inner_proj * value_proj).astype(BF16)
    halo_copy = remote(
        gated.at[pl.ds(rows - 16, 16), :], halo, halo_s.at[0], halo_r.at[0],
        lax.rem(e_me + 1, ep), t_me,
    )
    halo_copy.start()
    padded[8:, :] = gated[...].astype(F32)
    loads[6].wait()
    outer_proj = jnp.dot(nm[...], ow[...], preferred_element_type=F32)
    halo_copy.wait()
    before = halo[...].astype(F32)[8:16, :]
    padded[0:8, :] = jnp.where(e_me > 0, before, jnp.zeros_like(before))
    n_taps = taps.shape[0]
    mixed = taps[0:1, :] * padded[pl.ds(9 - n_taps, rows), :]
    for j in range(1, n_taps):
        mixed = mixed + taps[j : j + 1, :] * padded[pl.ds(9 - n_taps + j, rows), :]
    conv[...] = (outer_proj * mixed).astype(BF16)
    mix_share = rows // tp

    def parity_rows(ref, c, step, cols):
        return jnp.concatenate(
            [
                ref[pl.ds(pl.multiple_of((z * CORES + c) * step, step), step), cols]
                for z in range(zs)
            ],
            axis=0,
        )

    loads[7].wait()
    everything = slice(None)

    def partner_tile(cols):
        pair_out[:, cols] = jnp.dot(
            parity_rows(conv, c_no, mix_share, everything), mw[:, cols], preferred_element_type=F32
        ).astype(BF16)

    column_tiles(width, 512, partner_tile)
    pair_copy = remote(pair_out, pair_in, mp_s.at[0], mp_r.at[0], e_me, partner)
    go(pair_copy)

    def own_tile(cols):
        keep[:, cols] = jnp.dot(
            parity_rows(conv, c_me, mix_share, everything), mw[:, cols], preferred_element_type=F32
        )

    column_tiles(width, 512, own_tile)
    pair_copy.wait_recv()

    def sum_tile(cols):
        total = keep[:, cols] + pair_in[:, cols].astype(F32)
        keep[:, cols] = total
        pair_in[:, cols] = total.astype(BF16)

    column_tiles(width, 512, sum_tile)

    def z_rows(z, step):
        return pl.ds(pl.multiple_of(z * step, step), step)

    for z in z_peers:
        go(
            remote(
                pair_in.at[z_rows(z, mix_share), :], zin.at[z_me], mz_s.at[z], mz_r.at[z_me],
                e_me, z * CORES + c_me,
            )
        )

    for e in ep_peers:
        here = got.at[half_rows(c_me, e), :]
        remote(here, here, disp_s.at[e], disp_r.at[e], e, t_me).wait_recv()
        go(remote(here, here, fwd_s.at[e], fwd_r.at[e], e_me, partner))
    for e in ep_peers:
        remote(wgot.at[e], wgot.at[e], w_s.at[e], w_r.at[e], e, t_me).wait_recv()
    for c in range(CORES):
        for e in range(ep):
            wrow[c * span + e * half : c * span + (e + 1) * half, :] = wgot[
                e, c * half : (c + 1) * half, :
            ]
    for e in ep_peers:
        there = got.at[half_rows(c_no, e), :]
        remote(there, there, fwd_s.at[e], fwd_r.at[e], e_me, partner).wait_recv()

    hidden = gw.shape[2]
    arrived_lane = iota((2 * span, 128), 1)
    for k in range(experts_here):
        pltpu.make_async_copy(gate_w.at[k], gw.at[k], gate_sem.at[k]).wait()
        pltpu.make_async_copy(up_w.at[k], uw.at[k], up_sem.at[k]).wait()

    def expert(k, carry):
        gate = jnp.dot(got[...], gw[k], preferred_element_type=F32)
        up = jnp.dot(got[...], uw[k], preferred_element_type=F32)
        weight = jnp.sum(
            jnp.where(arrived_lane == e_me * experts_here + k, wrow[...], 0.0),
            axis=1, keepdims=True,
        )
        value = gate / (1.0 + jnp.exp(-gate)) * up * weight
        hid[k] = value.astype(BF16)
        return carry

    lax.fori_loop(0, experts_here, expert, 0)
    for k in range(experts_here):
        pltpu.make_async_copy(down_w.at[k], dw.at[k], down_sem.at[k]).wait()

    chunk = width // CHUNKS
    tile = min(512, chunk)

    def core_rows(c):
        return pl.ds(pl.multiple_of(c * span, span), span)

    def down(c, cols):
        total = jnp.dot(hid[0, core_rows(c), :], dw[0, :, cols], preferred_element_type=F32)
        for k in range(1, experts_here):
            total = total + jnp.dot(
                hid[k, core_rows(c), :], dw[k, :, cols], preferred_element_type=F32
            )
        return total

    y_copies = {}

    def stage_a(j):
        for i in range(chunk // tile):
            at = slice(i * tile, (i + 1) * tile)
            cols = slice(j * chunk + i * tile, j * chunk + (i + 1) * tile)
            y_out[j, :, at] = down(c_no, cols).astype(BF16)
        y_copies[j] = remote(y_out.at[j], y_in.at[j], yp_s.at[j], yp_r.at[j], e_me, partner)
        go(y_copies[j])
        for i in range(chunk // tile):
            at = slice(i * tile, (i + 1) * tile)
            cols = slice(j * chunk + i * tile, j * chunk + (i + 1) * tile)
            y_keep[j % 2, :, at] = down(c_me, cols)

    def e_rows(e):
        return pl.ds(pl.multiple_of(e * half, half), half)

    def stage_b(j):
        y_copies[j].wait_recv()
        y_in[j] = (y_keep[j % 2] + y_in[j].astype(F32)).astype(BF16)
        for e in ep_peers:
            go(
                remote(
                    y_in.at[j, e_rows(e), :], e_in.at[j, e_rows(e_me), :],
                    ye_s.at[j, e], ye_r.at[j, e_me], e, t_me,
                )
            )
        e_in[j, e_rows(e_me), :] = y_in[j, e_rows(e_me), :]

    def stage_c(j):
        for e in ep_peers:
            here = e_in.at[j, e_rows(e), :]
            remote(here, here, ye_s.at[j, e], ye_r.at[j, e], e, t_me).wait_recv()
        own = parity_rows(spread, c_me, share, core_rows(c_me))
        total = jnp.dot(own, e_in[j], preferred_element_type=F32)
        s_out[j] = total.astype(BF16)
        for z in z_peers:
            go(
                remote(
                    s_out.at[j, z_rows(z, share), :], s_in.at[j, z_me],
                    yz_s.at[j, z], yz_r.at[j, z_me], e_me, z * CORES + c_me,
                )
            )
        s_keep[j % 2] = total

    def stage_d(j):
        total = s_keep[j % 2, z_rows(z_me, share), :]
        for z in z_peers:
            here = s_in.at[j, z]
            remote(here, here, yz_s.at[j, z], yz_r.at[j, z], e_me, z * CORES + c_me).wait_recv()
            total = total + s_in[j, z].astype(F32)
        expert_out[:, j * chunk : (j + 1) * chunk] = total.astype(BF16)

    for j in range(CHUNKS):
        stage_a(j)
        if j:
            stage_b(j - 1)
    stage_b(CHUNKS - 1)

    total = keep[z_rows(z_me, mix_share), :]
    for z in z_peers:
        here = zin.at[z]
        remote(here, here, mz_s.at[z], mz_r.at[z], e_me, z * CORES + c_me).wait_recv()
        total = total + zin[z].astype(F32)
    mixer_out[...] = total.astype(BF16)

    for j in range(CHUNKS):
        stage_c(j)
        if j:
            stage_d(j - 1)
    stage_d(CHUNKS - 1)
    for copy in sends:
        copy.wait_send()


def local(ep, tp, *args):
    (mix_tokens, mix_gain, value_w, inner_w, outer_w, taps, mix_w, moe_tokens, moe_gain,
     router_group, router_expert, routes, gate_w, up_w, down_w) = args
    rows, width = mix_tokens.shape
    count = moe_tokens.shape[0]
    channels, hidden = value_w.shape[1], gate_w.shape[2]
    experts_here = gate_w.shape[0]
    zs = tp // CORES
    share, mix_share = count // tp, rows // tp
    topk = routes.shape[1]
    slots = experts_here * CAP
    if experts_here % EPG == 0:
        slots = slots // topk
    slots = min(slots, share)
    half = zs * slots
    span = ep * half
    chunk = width // CHUNKS
    any_ref = pl.BlockSpec(memory_space=pl.ANY)
    vmem = pl.BlockSpec(memory_space=pltpu.VMEM)
    V, D = pltpu.VMEM, lambda *s: pltpu.SemaphoreType.DMA(s)
    scratch = [
        V((rows, width), BF16), V((count, width), BF16),
        V(router_group.shape, BF16), V(router_expert.shape, BF16),
        V(value_w.shape, BF16), V(inner_w.shape, BF16), V(outer_w.shape, BF16),
        V(mix_w.shape, BF16),
        V(gate_w.shape, BF16), V(up_w.shape, BF16), V(down_w.shape, BF16),
        V((rows, width), BF16), V((count, width), BF16), V((count, 2 * span), BF16),
        V((2 * span, width), BF16), V((2 * span, width), BF16),
        V((ep, 2 * half, 128), F32), V((ep, 2 * half, 128), F32), V((2 * span, 128), F32),
        V((rows, channels), BF16), V((16, channels), BF16), V((rows + 8, channels), F32),
        V((rows, channels), BF16),
        V((zs * mix_share, width), BF16), V((zs * mix_share, width), BF16),
        V((zs * mix_share, width), F32),
        V((zs, mix_share, width), BF16),
        V((experts_here, 2 * span, hidden), BF16),
        V((CHUNKS, span, chunk), BF16), V((CHUNKS, span, chunk), BF16),
        V((2, span, chunk), F32),
        V((CHUNKS, span, chunk), BF16),
        V((2, zs * share, chunk), F32), V((CHUNKS, zs * share, chunk), BF16),
        V((CHUNKS, zs, share, chunk), BF16),
        D(8), D(experts_here), D(experts_here), D(experts_here),
        D(ep), D(ep), D(ep), D(ep), D(ep), D(ep), D(1), D(1), D(1), D(1), D(zs), D(zs),
        D(CHUNKS), D(CHUNKS), D(CHUNKS, ep), D(CHUNKS, ep), D(CHUNKS, zs), D(CHUNKS, zs),
    ]
    out = [
        jax.ShapeDtypeStruct((mix_share, width), BF16),
        jax.ShapeDtypeStruct((share, width), BF16),
    ]
    in_specs = [
        any_ref, vmem, any_ref, any_ref, any_ref, vmem, any_ref, any_ref, vmem,
        any_ref, any_ref, vmem, any_ref, any_ref, any_ref,
    ]
    return pl.pallas_call(
        functools.partial(kernel, (ep, tp, zs, half, experts_here)),
        out_shape=out,
        in_specs=in_specs,
        out_specs=[vmem, vmem],
        scratch_shapes=scratch,
        compiler_params=pltpu.CompilerParams(
            collective_id=0, has_side_effects=True, vmem_limit_bytes=67043328
        ),
        name="mixer_and_experts",
    )(
        mix_tokens, mix_gain.reshape(1, width), value_w, inner_w, outer_w, taps, mix_w,
        moe_tokens, moe_gain.reshape(1, width), router_group, router_expert, routes,
        gate_w, up_w, down_w,
    )


def solution(mesh):
    return jax.shard_map(
        lambda *args: tuple(local(mesh.shape["ep"], mesh.shape["tp"], *args)),
        mesh=mesh,
        in_specs=(
            P("ep", None), P(), P(None, "tp"), P(None, "tp"), P(None, "tp"), P(None, "tp"),
            P("tp", None), P("ep", None), P(), P(), P(), P("ep", None),
            P("ep", None, "tp"), P("ep", None, "tp"), P("ep", "tp", None),
        ),
        out_specs=(P(("ep", "tp"), None), P(("ep", "tp"), None)),
        check_vma=False,
    )
```

```python
import functools

import jax
import jax.numpy as jnp
from jax import lax
from jax.experimental import pallas as pl
from jax.experimental.pallas import tpu as pltpu
from jax.sharding import PartitionSpec as P

EPG = 4
CAP = 4
CORES = 2
CHUNKS = 8
PARTS = 4
MESH = pl.DeviceIdType.MESH
F32, BF16 = jnp.float32, jnp.bfloat16


def iota(shape, dim):
    return lax.broadcasted_iota(jnp.int32, shape, dim)


def norm_rows(src, gain, dst):
    width = src.shape[1]

    def body(i, carry):
        rows = pl.ds(pl.multiple_of(i * 16, 16), 16)
        x = src[rows, :].astype(F32)
        inv = lax.rsqrt(jnp.sum(x * x, axis=1, keepdims=True) * (1.0 / width) + 1e-06)
        dst[rows, :] = (x * inv * gain[...]).astype(BF16)
        return carry

    lax.fori_loop(0, src.shape[0] // 16, body, 0)


def column_tiles(width, tile, body):
    def step(i, carry):
        body(pl.ds(pl.multiple_of(i * tile, tile), tile))
        return carry

    lax.fori_loop(0, width // tile, step, 0)


def kernel(
    cfg,
    mix_tokens, mix_gain, value_w, inner_w, outer_w, taps, mix_w, moe_tokens, moe_gain,
    router_group, router_expert, routes, gate_w, up_w, down_w,
    mixer_out, expert_out,
    xm, xe, rg, rx, vw, iw, ow, mw, gw, uw, dw,
    nm, ne, spread, gather, pack, got, wpack, wgot, wrow,
    gated, halo, padded, conv, ordered, pair_out, pair_in, keep, zin,
    gate_acc, up_acc, hid, both_y, y_out, y_in, y_keep, e_in, s_keep, s_out, s_in,
    load_sem, gate_sem, up_sem, down_sem,
    disp_s, disp_r, w_s, w_r, fwd_s, fwd_r, halo_s, halo_r, mp_s, mp_r, mz_s, mz_r,
    yp_s, yp_r, ye_s, ye_r, yz_s, yz_r,
):
    ep, tp, zs, half, experts_here = cfg
    e_me, t_me = lax.axis_index("ep"), lax.axis_index("tp")
    z_me, c_me = t_me // CORES, lax.rem(t_me, CORES)
    c_no = 1 - c_me
    partner = z_me * CORES + c_no
    width = xm.shape[1]
    ep_peers = [lax.rem(e_me + d, ep) for d in range(1, ep)]
    z_peers = [lax.rem(z_me + d, zs) for d in range(1, zs)]

    barrier = pltpu.get_barrier_semaphore()
    for e in ep_peers:
        pl.semaphore_signal(barrier, inc=1, device_id={"ep": e, "tp": t_me}, device_id_type=MESH)
    for z in z_peers:
        pl.semaphore_signal(
            barrier, inc=1, device_id={"ep": e_me, "tp": z * CORES + c_me}, device_id_type=MESH
        )
    pl.semaphore_signal(barrier, inc=1, device_id={"ep": e_me, "tp": partner}, device_id_type=MESH)

    def load(k, src, dst):
        return pltpu.make_async_copy(src, dst, load_sem.at[k])

    loads = [
        load(k, s, d)
        for k, (s, d) in enumerate(
            [
                (moe_tokens, xe), (router_group, rg), (router_expert, rx), (mix_tokens, xm),
                (value_w, vw), (inner_w, iw), (outer_w, ow), (mix_w, mw),
            ]
        )
    ]
    for c in loads:
        c.start()

    def remote(src, dst, s_sem, r_sem, e, t):
        return pltpu.make_async_remote_copy(
            src_ref=src, dst_ref=dst, send_sem=s_sem, recv_sem=r_sem,
            device_id={"ep": e, "tp": t}, device_id_type=MESH,
        )

    count = xe.shape[0]
    share = count // tp
    slots = half // zs
    span = ep * half
    diagonal = jnp.where(iota((count, count), 0) == iota((count, count), 1), 1.0, 0.0)
    r = lax.dot_general(
        diagonal.astype(BF16), routes[...].astype(F32).astype(BF16), (((1,), (1,)), ((), ())),
        preferred_element_type=F32,
    ).astype(jnp.int32)
    picks = [r[:, 0:1], r[:, 1:2]]
    lane = iota((count, 128), 1)
    shards = [
        sum((p >= s * experts_here).astype(jnp.int32) for s in range(1, ep)) for p in picks
    ]
    member = jnp.where((lane == shards[0]) | (lane == shards[1]), 1.0, 0.0).astype(BF16)
    ti, tj = iota((count, count), 0), iota((count, count), 1)
    earlier = jnp.where(((ti ^ tj) < share) & (tj < ti), 1.0, 0.0).astype(BF16)
    rank = jnp.dot(earlier, member, preferred_element_type=F32)
    block = lax.shift_right_logical(iota((count, 1), 0), share.bit_length() - 1)
    base = (block & 1) * span + lax.shift_right_logical(block, 1) * slots
    slot_lane = iota((count, 2 * span), 1)
    hits = []
    for s in shards:
        mine = jnp.sum(jnp.where(lane == s, rank, 0.0), axis=1, keepdims=True).astype(jnp.int32)
        hits.append(slot_lane == base + s * half + mine)
    one_hot = jnp.where(hits[0] | hits[1], 1.0, 0.0).astype(BF16)
    spread[...] = one_hot
    gather[...] = lax.dot_general(
        one_hot, diagonal.astype(BF16), (((0,), (0,)), ((), ())), preferred_element_type=F32
    ).astype(BF16)
    loads[0].wait()
    norm_rows(xe, moe_gain, ne)
    part = width // PARTS

    def pack_part(q):
        cols = slice(q * part, (q + 1) * part)
        pack[:, cols] = jnp.dot(
            gather[...], ne[:, cols], preferred_element_type=F32
        ).astype(BF16)

    pack_part(0)
    pl.semaphore_wait(barrier, (ep - 1) + (zs - 1) + 1)
    sends = []

    def go(copy):
        copy.start()
        sends.append(copy)

    def half_rows(c, e):
        return pl.ds(pl.multiple_of(c * span + e * half, half), half)

    def dispatch(q):
        cols = pl.ds(q * part, part)
        for e in ep_peers:
            go(
                remote(
                    pack.at[half_rows(c_me, e), cols], got.at[half_rows(c_me, e_me), cols],
                    disp_s.at[q, e], disp_r.at[q, e_me], e, t_me,
                )
            )

    early = PARTS // 2
    for q in range(1, PARTS):
        if q <= early:
            dispatch(q - 1)
        pack_part(q)
    for k in range(experts_here):
        pltpu.make_async_copy(gate_w.at[k], gw.at[k], gate_sem.at[k]).start()
        pltpu.make_async_copy(up_w.at[k], uw.at[k], up_sem.at[k]).start()
    for k in range(experts_here):
        pltpu.make_async_copy(down_w.at[k], dw.at[k], down_sem.at[k]).start()

    loads[1].wait()
    loads[2].wait()
    lanes = (((1,), (1,)), ((), ()))
    group_exp = jnp.exp(lax.dot_general(ne[...], rg[...], lanes, preferred_element_type=F32))
    expert_logit = lax.dot_general(ne[...], rx[...], lanes, preferred_element_type=F32)
    groups, experts = group_exp.shape[1], expert_logit.shape[1]
    group = sum((picks[0] >= s * EPG).astype(jnp.int32) for s in range(1, groups))
    chosen_group = jnp.where(iota((count, groups), 1) == group, group_exp, 0.0)
    group_gate = jnp.sum(chosen_group, axis=1, keepdims=True) / jnp.sum(
        group_exp, axis=1, keepdims=True
    )
    expert_lane = iota((count, experts), 1)
    chosen = [
        jnp.exp(jnp.sum(jnp.where(expert_lane == p, expert_logit, 0.0), axis=1, keepdims=True))
        for p in picks
    ]
    scale = chosen[0] + chosen[1]
    weights = sum(
        jnp.where(lane == p, group_gate * c / scale, 0.0) for p, c in zip(picks, chosen)
    )
    parts, rest = [], weights
    for _ in range(3):
        parts.append(rest.astype(BF16))
        rest = rest - parts[-1].astype(F32)
    packed_w = sum(jnp.dot(gather[...], p, preferred_element_type=F32) for p in parts)
    for e in range(ep):
        for c in range(CORES):
            wpack[e, c * half : (c + 1) * half, :] = packed_w[
                c * span + e * half : c * span + (e + 1) * half, :
            ]
    wgot[e_me] = wpack[e_me]
    for c in range(CORES):
        got[half_rows(c, e_me), :] = pack[half_rows(c, e_me), :]

    loads[3].wait()
    norm_rows(xm, mix_gain, nm)
    loads[4].wait()
    loads[5].wait()
    rows = xm.shape[0]
    value_proj = jnp.dot(nm[...], vw[...], preferred_element_type=F32)
    inner_proj = jnp.dot(nm[...], iw[...], preferred_element_type=F32)
    gated[...] = (inner_proj * value_proj).astype(BF16)
    halo_copy = remote(
        gated.at[pl.ds(rows - 16, 16), :], halo, halo_s.at[0], halo_r.at[0],
        lax.rem(e_me + 1, ep), t_me,
    )
    halo_copy.start()
    for q in range(early, PARTS):
        dispatch(q)
        if q == early:
            for e in ep_peers:
                go(remote(wpack.at[e], wgot.at[e_me], w_s.at[e], w_r.at[e_me], e, t_me))
    padded[8:, :] = gated[...].astype(F32)
    loads[6].wait()
    outer_proj = jnp.dot(nm[...], ow[...], preferred_element_type=F32)
    halo_copy.wait()
    before = halo[...].astype(F32)[8:16, :]
    padded[0:8, :] = jnp.where(e_me > 0, before, jnp.zeros_like(before))
    n_taps = taps.shape[0]
    mixed = taps[0:1, :] * padded[pl.ds(9 - n_taps, rows), :]
    for j in range(1, n_taps):
        mixed = mixed + taps[j : j + 1, :] * padded[pl.ds(9 - n_taps + j, rows), :]
    conv[...] = (outer_proj * mixed).astype(BF16)
    mix_share = rows // tp

    def parity_rows(ref, c, step, cols):
        return jnp.concatenate(
            [
                ref[pl.ds(pl.multiple_of((z * CORES + c) * step, step), step), cols]
                for z in range(zs)
            ],
            axis=0,
        )

    loads[7].wait()
    everything = slice(None)

    mix_rows = zs * mix_share
    ordered[0:mix_rows, :] = parity_rows(conv, c_no, mix_share, everything)
    ordered[mix_rows:, :] = parity_rows(conv, c_me, mix_share, everything)

    def mix_tile(cols):
        both = jnp.dot(ordered[...], mw[:, cols], preferred_element_type=F32)
        pair_out[:, cols] = both[0:mix_rows].astype(BF16)
        keep[:, cols] = both[mix_rows:]

    column_tiles(width, 512, mix_tile)
    pair_copy = remote(pair_out, pair_in, mp_s.at[0], mp_r.at[0], e_me, partner)
    go(pair_copy)
    pair_copy.wait_recv()

    def sum_tile(cols):
        total = keep[:, cols] + pair_in[:, cols].astype(F32)
        keep[:, cols] = total
        pair_in[:, cols] = total.astype(BF16)

    column_tiles(width, 512, sum_tile)

    def z_rows(z, step):
        return pl.ds(pl.multiple_of(z * step, step), step)

    for z in z_peers:
        go(
            remote(
                pair_in.at[z_rows(z, mix_share), :], zin.at[z_me], mz_s.at[z], mz_r.at[z_me],
                e_me, z * CORES + c_me,
            )
        )

    def forward(q):
        cols = pl.ds(q * part, part)
        for e in ep_peers:
            here = got.at[half_rows(c_me, e), cols]
            remote(here, here, disp_s.at[q, e], disp_r.at[q, e], e, t_me).wait_recv()
            go(remote(here, here, fwd_s.at[q, e], fwd_r.at[q, e], e_me, partner))

    def forwarded(q):
        cols = pl.ds(q * part, part)
        for e in ep_peers:
            there = got.at[half_rows(c_no, e), cols]
            remote(there, there, fwd_s.at[q, e], fwd_r.at[q, e], e_me, partner).wait_recv()

    arrived_lane = iota((2 * span, 128), 1)

    def project(q):
        cols = slice(q * part, (q + 1) * part)

        def expert(k, carry):
            gate = jnp.dot(got[:, cols], gw[k, cols, :], preferred_element_type=F32)
            up = jnp.dot(got[:, cols], uw[k, cols, :], preferred_element_type=F32)
            if q:
                gate = gate + gate_acc[k]
                up = up + up_acc[k]
            if q < PARTS - 1:
                gate_acc[k] = gate
                up_acc[k] = up
                return carry
            weight = jnp.sum(
                jnp.where(arrived_lane == e_me * experts_here + k, wrow[...], 0.0),
                axis=1, keepdims=True,
            )
            hid[k] = (gate / (1.0 + jnp.exp(-gate)) * up * weight).astype(BF16)
            return carry

        lax.fori_loop(0, experts_here, expert, 0)

    forward(0)
    for k in range(experts_here):
        pltpu.make_async_copy(gate_w.at[k], gw.at[k], gate_sem.at[k]).wait()
        pltpu.make_async_copy(up_w.at[k], uw.at[k], up_sem.at[k]).wait()
    for q in range(PARTS):
        if q + 1 < PARTS:
            forward(q + 1)
        else:
            for e in ep_peers:
                remote(wgot.at[e], wgot.at[e], w_s.at[e], w_r.at[e], e, t_me).wait_recv()
            for c in range(CORES):
                for e in range(ep):
                    wrow[c * span + e * half : c * span + (e + 1) * half, :] = wgot[
                        e, c * half : (c + 1) * half, :
                    ]
        forwarded(q)
        project(q)
    for k in range(experts_here):
        pltpu.make_async_copy(down_w.at[k], dw.at[k], down_sem.at[k]).wait()

    chunk = width // CHUNKS
    tile = min(512, chunk)

    def core_rows(c):
        return pl.ds(pl.multiple_of(c * span, span), span)

    y_copies = {}

    def stage_a(j):
        for i in range(chunk // tile):
            at = slice(i * tile, (i + 1) * tile)
            cols = slice(j * chunk + i * tile, j * chunk + (i + 1) * tile)
            both = jnp.dot(hid[0], dw[0, :, cols], preferred_element_type=F32)
            for k in range(1, experts_here):
                both = both + jnp.dot(hid[k], dw[k, :, cols], preferred_element_type=F32)
            both_y[...] = both
            y_out[j, :, at] = both_y[core_rows(c_no), :].astype(BF16)
            y_keep[j % 2, :, at] = both_y[core_rows(c_me), :]
        y_copies[j] = remote(y_out.at[j], y_in.at[j], yp_s.at[j], yp_r.at[j], e_me, partner)
        go(y_copies[j])

    def e_rows(e):
        return pl.ds(pl.multiple_of(e * half, half), half)

    def stage_b(j):
        y_copies[j].wait_recv()
        y_in[j] = (y_keep[j % 2] + y_in[j].astype(F32)).astype(BF16)
        for e in ep_peers:
            go(
                remote(
                    y_in.at[j, e_rows(e), :], e_in.at[j, e_rows(e_me), :],
                    ye_s.at[j, e], ye_r.at[j, e_me], e, t_me,
                )
            )
        e_in[j, e_rows(e_me), :] = y_in[j, e_rows(e_me), :]

    def stage_c(j):
        for e in ep_peers:
            here = e_in.at[j, e_rows(e), :]
            remote(here, here, ye_s.at[j, e], ye_r.at[j, e], e, t_me).wait_recv()
        own = parity_rows(spread, c_me, share, core_rows(c_me))
        total = jnp.dot(own, e_in[j], preferred_element_type=F32)
        s_out[j] = total.astype(BF16)
        for z in z_peers:
            go(
                remote(
                    s_out.at[j, z_rows(z, share), :], s_in.at[j, z_me],
                    yz_s.at[j, z], yz_r.at[j, z_me], e_me, z * CORES + c_me,
                )
            )
        s_keep[j % 4] = total

    def stage_d(j):
        total = s_keep[j % 4, z_rows(z_me, share), :]
        for z in z_peers:
            here = s_in.at[j, z]
            remote(here, here, yz_s.at[j, z], yz_r.at[j, z], e_me, z * CORES + c_me).wait_recv()
            total = total + s_in[j, z].astype(F32)
        expert_out[:, j * chunk : (j + 1) * chunk] = total.astype(BF16)

    for j in range(CHUNKS):
        stage_a(j)
        if j:
            stage_b(j - 1)
    stage_b(CHUNKS - 1)

    total = keep[z_rows(z_me, mix_share), :]
    for z in z_peers:
        here = zin.at[z]
        remote(here, here, mz_s.at[z], mz_r.at[z], e_me, z * CORES + c_me).wait_recv()
        total = total + zin[z].astype(F32)
    mixer_out[...] = total.astype(BF16)

    lag = 3
    for j in range(CHUNKS + lag):
        if j < CHUNKS:
            stage_c(j)
        if j >= lag:
            stage_d(j - lag)
    for copy in sends:
        copy.wait_send()


def local(ep, tp, *args):
    (mix_tokens, mix_gain, value_w, inner_w, outer_w, taps, mix_w, moe_tokens, moe_gain,
     router_group, router_expert, routes, gate_w, up_w, down_w) = args
    rows, width = mix_tokens.shape
    count = moe_tokens.shape[0]
    channels, hidden = value_w.shape[1], gate_w.shape[2]
    experts_here = gate_w.shape[0]
    zs = tp // CORES
    share, mix_share = count // tp, rows // tp
    topk = routes.shape[1]
    slots = experts_here * CAP
    if experts_here % EPG == 0:
        slots = slots // topk
    slots = min(slots, share)
    half = zs * slots
    span = ep * half
    chunk = width // CHUNKS
    any_ref = pl.BlockSpec(memory_space=pl.ANY)
    vmem = pl.BlockSpec(memory_space=pltpu.VMEM)
    V, D = pltpu.VMEM, lambda *s: pltpu.SemaphoreType.DMA(s)
    scratch = [
        V((rows, width), BF16), V((count, width), BF16),
        V(router_group.T.shape, BF16), V(router_expert.T.shape, BF16),
        V(value_w.shape, BF16), V(inner_w.shape, BF16), V(outer_w.shape, BF16),
        V(mix_w.shape, BF16),
        V(gate_w.shape, BF16), V(up_w.shape, BF16), V(down_w.shape, BF16),
        V((rows, width), BF16), V((count, width), BF16), V((count, 2 * span), BF16), V((2 * span, count), BF16),
        V((2 * span, width), BF16), V((2 * span, width), BF16),
        V((ep, 2 * half, 128), F32), V((ep, 2 * half, 128), F32), V((2 * span, 128), F32),
        V((rows, channels), BF16), V((16, channels), BF16), V((rows + 8, channels), F32),
        V((rows, channels), BF16), V((rows, channels), BF16),
        V((zs * mix_share, width), BF16), V((zs * mix_share, width), BF16),
        V((zs * mix_share, width), F32),
        V((zs, mix_share, width), BF16),
        V((experts_here, 2 * span, hidden), F32), V((experts_here, 2 * span, hidden), F32),
        V((experts_here, 2 * span, hidden), BF16), V((2 * span, min(512, chunk)), F32),
        V((CHUNKS, span, chunk), BF16), V((CHUNKS, span, chunk), BF16),
        V((2, span, chunk), F32),
        V((CHUNKS, span, chunk), BF16),
        V((4, zs * share, chunk), F32), V((CHUNKS, zs * share, chunk), BF16),
        V((CHUNKS, zs, share, chunk), BF16),
        D(8), D(experts_here), D(experts_here), D(experts_here),
        D(PARTS, ep), D(PARTS, ep), D(ep), D(ep), D(PARTS, ep), D(PARTS, ep), D(1), D(1), D(1), D(1), D(zs), D(zs),
        D(CHUNKS), D(CHUNKS), D(CHUNKS, ep), D(CHUNKS, ep), D(CHUNKS, zs), D(CHUNKS, zs),
    ]
    out = [
        jax.ShapeDtypeStruct((mix_share, width), BF16),
        jax.ShapeDtypeStruct((share, width), BF16),
    ]
    in_specs = [
        any_ref, vmem, any_ref, any_ref, any_ref, vmem, any_ref, any_ref, vmem,
        any_ref, any_ref, vmem, any_ref, any_ref, any_ref,
    ]
    return pl.pallas_call(
        functools.partial(kernel, (ep, tp, zs, half, experts_here)),
        out_shape=out,
        in_specs=in_specs,
        out_specs=[vmem, vmem],
        scratch_shapes=scratch,
        compiler_params=pltpu.CompilerParams(
            collective_id=0, has_side_effects=True, vmem_limit_bytes=67043328
        ),
        name="mixer_and_experts",
    )(
        mix_tokens, mix_gain.reshape(1, width), value_w, inner_w, outer_w, taps, mix_w,
        moe_tokens, moe_gain.reshape(1, width), router_group.T, router_expert.T, routes.T,
        gate_w, up_w, down_w,
    )


def solution(mesh):
    return jax.shard_map(
        lambda *args: tuple(local(mesh.shape["ep"], mesh.shape["tp"], *args)),
        mesh=mesh,
        in_specs=(
            P("ep", None), P(), P(None, "tp"), P(None, "tp"), P(None, "tp"), P(None, "tp"),
            P("tp", None), P("ep", None), P(), P(), P(), P("ep", None),
            P("ep", None, "tp"), P("ep", None, "tp"), P("ep", "tp", None),
        ),
        out_specs=(P(("ep", "tp"), None), P(("ep", "tp"), None)),
        check_vma=False,
    )
```

```python
import functools

import jax
import jax.numpy as jnp
from jax import lax
from jax.experimental import pallas as pl
from jax.experimental.pallas import tpu as pltpu
from jax.sharding import PartitionSpec as P

EPG = 4
CAP = 4
CORES = 2
CHUNKS = 8
SPLIT = (2, 2, 3, 1)
PARTS = len(SPLIT)
MESH = pl.DeviceIdType.MESH
F32, BF16 = jnp.float32, jnp.bfloat16


def iota(shape, dim):
    return lax.broadcasted_iota(jnp.int32, shape, dim)


def norm_rows(src, gain, dst):
    width = src.shape[1]

    def body(i, carry):
        rows = pl.ds(pl.multiple_of(i * 16, 16), 16)
        x = src[rows, :].astype(F32)
        inv = lax.rsqrt(jnp.sum(x * x, axis=1, keepdims=True) * (1.0 / width) + 1e-06)
        dst[rows, :] = (x * inv * gain[...]).astype(BF16)
        return carry

    lax.fori_loop(0, src.shape[0] // 16, body, 0)


def column_tiles(width, tile, body):
    def step(i, carry):
        body(pl.ds(pl.multiple_of(i * tile, tile), tile))
        return carry

    lax.fori_loop(0, width // tile, step, 0)


def kernel(
    cfg,
    mix_tokens, mix_gain, value_w, inner_w, outer_w, taps, mix_w, moe_tokens, moe_gain,
    router_group, router_expert, routes, gate_w, up_w, down_w,
    mixer_out, expert_out,
    xm, xe, rg, rx, vw, iw, ow, mw, gw, uw, dw,
    nm, ne, spread, gather, pack, got, wpack, wgot, wrow,
    gated, halo, padded, conv, ordered, pair_out, pair_in, keep, zin,
    gate_acc, up_acc, hid, both_y, y_out, y_in, y_keep, e_in, s_keep, s_out, s_in,
    load_sem, gate_sem, up_sem, down_sem,
    disp_s, disp_r, w_s, w_r, fwd_s, fwd_r, halo_s, halo_r, mp_s, mp_r, mz_s, mz_r,
    yp_s, yp_r, ye_s, ye_r, yz_s, yz_r,
):
    ep, tp, zs, half, experts_here = cfg
    e_me, t_me = lax.axis_index("ep"), lax.axis_index("tp")
    z_me, c_me = t_me // CORES, lax.rem(t_me, CORES)
    c_no = 1 - c_me
    partner = z_me * CORES + c_no
    width = xm.shape[1]
    ep_peers = [lax.rem(e_me + d, ep) for d in range(1, ep)]
    z_peers = [lax.rem(z_me + d, zs) for d in range(1, zs)]

    barrier = pltpu.get_barrier_semaphore()
    for e in ep_peers:
        pl.semaphore_signal(barrier, inc=1, device_id={"ep": e, "tp": t_me}, device_id_type=MESH)
    for z in z_peers:
        pl.semaphore_signal(
            barrier, inc=1, device_id={"ep": e_me, "tp": z * CORES + c_me}, device_id_type=MESH
        )
    pl.semaphore_signal(barrier, inc=1, device_id={"ep": e_me, "tp": partner}, device_id_type=MESH)

    def load(k, src, dst):
        return pltpu.make_async_copy(src, dst, load_sem.at[k])

    loads = [
        load(k, s, d)
        for k, (s, d) in enumerate(
            [
                (moe_tokens, xe), (router_group, rg), (router_expert, rx), (mix_tokens, xm),
                (value_w, vw), (inner_w, iw), (outer_w, ow), (mix_w, mw),
            ]
        )
    ]
    for c in loads:
        c.start()

    def remote(src, dst, s_sem, r_sem, e, t):
        return pltpu.make_async_remote_copy(
            src_ref=src, dst_ref=dst, send_sem=s_sem, recv_sem=r_sem,
            device_id={"ep": e, "tp": t}, device_id_type=MESH,
        )

    count = xe.shape[0]
    share = count // tp
    slots = half // zs
    span = ep * half
    diagonal = jnp.where(iota((count, count), 0) == iota((count, count), 1), 1.0, 0.0)
    r = lax.dot_general(
        diagonal.astype(BF16), routes[...].astype(F32).astype(BF16), (((1,), (1,)), ((), ())),
        preferred_element_type=F32,
    ).astype(jnp.int32)
    picks = [r[:, 0:1], r[:, 1:2]]
    lane = iota((count, 128), 1)
    shards = [
        sum((p >= s * experts_here).astype(jnp.int32) for s in range(1, ep)) for p in picks
    ]
    member = jnp.where((lane == shards[0]) | (lane == shards[1]), 1.0, 0.0).astype(BF16)
    ti, tj = iota((count, count), 0), iota((count, count), 1)
    earlier = jnp.where(((ti ^ tj) < share) & (tj < ti), 1.0, 0.0).astype(BF16)
    rank = jnp.dot(earlier, member, preferred_element_type=F32)
    block = lax.shift_right_logical(iota((count, 1), 0), share.bit_length() - 1)
    base = (block & 1) * span + lax.shift_right_logical(block, 1) * slots
    slot_lane = iota((count, 2 * span), 1)
    hits = []
    for s in shards:
        mine = jnp.sum(jnp.where(lane == s, rank, 0.0), axis=1, keepdims=True).astype(jnp.int32)
        hits.append(slot_lane == base + s * half + mine)
    one_hot = jnp.where(hits[0] | hits[1], 1.0, 0.0).astype(BF16)
    spread[...] = one_hot
    gather[...] = lax.dot_general(
        one_hot, diagonal.astype(BF16), (((0,), (0,)), ((), ())), preferred_element_type=F32
    ).astype(BF16)
    loads[0].wait()
    norm_rows(xe, moe_gain, ne)
    unit = width // sum(SPLIT)

    def part_slice(q):
        return sum(SPLIT[:q]) * unit, SPLIT[q] * unit

    def pack_part(q):
        first, size = part_slice(q)
        cols = slice(first, first + size)
        pack[:, cols] = jnp.dot(
            gather[...], ne[:, cols], preferred_element_type=F32
        ).astype(BF16)

    pack_part(0)
    pl.semaphore_wait(barrier, (ep - 1) + (zs - 1) + 1)
    sends = []

    def go(copy):
        copy.start()
        sends.append(copy)

    def half_rows(c, e):
        return pl.ds(pl.multiple_of(c * span + e * half, half), half)

    def dispatch(q):
        cols = pl.ds(*part_slice(q))
        for e in ep_peers:
            go(
                remote(
                    pack.at[half_rows(c_me, e), cols], got.at[half_rows(c_me, e_me), cols],
                    disp_s.at[q, e], disp_r.at[q, e_me], e, t_me,
                )
            )

    early = PARTS // 2
    for q in range(1, PARTS):
        if q <= early:
            dispatch(q - 1)
        pack_part(q)
    for k in range(experts_here):
        pltpu.make_async_copy(gate_w.at[k], gw.at[k], gate_sem.at[k]).start()
        pltpu.make_async_copy(up_w.at[k], uw.at[k], up_sem.at[k]).start()
    for k in range(experts_here):
        pltpu.make_async_copy(down_w.at[k], dw.at[k], down_sem.at[k]).start()

    loads[1].wait()
    loads[2].wait()
    lanes = (((1,), (1,)), ((), ()))
    group_exp = jnp.exp(lax.dot_general(ne[...], rg[...], lanes, preferred_element_type=F32))
    expert_logit = lax.dot_general(ne[...], rx[...], lanes, preferred_element_type=F32)
    groups, experts = group_exp.shape[1], expert_logit.shape[1]
    group = sum((picks[0] >= s * EPG).astype(jnp.int32) for s in range(1, groups))
    chosen_group = jnp.where(iota((count, groups), 1) == group, group_exp, 0.0)
    group_gate = jnp.sum(chosen_group, axis=1, keepdims=True) / jnp.sum(
        group_exp, axis=1, keepdims=True
    )
    expert_lane = iota((count, experts), 1)
    chosen = [
        jnp.exp(jnp.sum(jnp.where(expert_lane == p, expert_logit, 0.0), axis=1, keepdims=True))
        for p in picks
    ]
    scale = chosen[0] + chosen[1]
    weights = sum(
        jnp.where(lane == p, group_gate * c / scale, 0.0) for p, c in zip(picks, chosen)
    )
    parts, rest = [], weights
    for _ in range(3):
        parts.append(rest.astype(BF16))
        rest = rest - parts[-1].astype(F32)
    packed_w = sum(jnp.dot(gather[...], p, preferred_element_type=F32) for p in parts)
    for e in range(ep):
        for c in range(CORES):
            wpack[e, c * half : (c + 1) * half, :] = packed_w[
                c * span + e * half : c * span + (e + 1) * half, :
            ]
    wgot[e_me] = wpack[e_me]
    for c in range(CORES):
        got[half_rows(c, e_me), :] = pack[half_rows(c, e_me), :]

    loads[3].wait()
    norm_rows(xm, mix_gain, nm)
    loads[4].wait()
    loads[5].wait()
    rows = xm.shape[0]
    value_proj = jnp.dot(nm[...], vw[...], preferred_element_type=F32)
    inner_proj = jnp.dot(nm[...], iw[...], preferred_element_type=F32)
    gated[...] = (inner_proj * value_proj).astype(BF16)
    halo_copy = remote(
        gated.at[pl.ds(rows - 16, 16), :], halo, halo_s.at[0], halo_r.at[0],
        lax.rem(e_me + 1, ep), t_me,
    )
    halo_copy.start()
    for q in range(early, PARTS):
        dispatch(q)
        if q == early:
            for e in ep_peers:
                go(remote(wpack.at[e], wgot.at[e_me], w_s.at[e], w_r.at[e_me], e, t_me))
    padded[8:, :] = gated[...].astype(F32)
    loads[6].wait()
    outer_proj = jnp.dot(nm[...], ow[...], preferred_element_type=F32)
    mix_share = rows // tp
    mix_rows = zs * mix_share
    everything = slice(None)
    pair_copy = remote(pair_out, pair_in, mp_s.at[0], mp_r.at[0], e_me, partner)

    def parity_rows(ref, c, step, cols):
        return jnp.concatenate(
            [
                ref[pl.ds(pl.multiple_of((z * CORES + c) * step, step), step), cols]
                for z in range(zs)
            ],
            axis=0,
        )

    def z_rows(z, step):
        return pl.ds(pl.multiple_of(z * step, step), step)

    def mixer_pair():
        halo_copy.wait()
        before = halo[...].astype(F32)[8:16, :]
        padded[0:8, :] = jnp.where(e_me > 0, before, jnp.zeros_like(before))
        n_taps = taps.shape[0]
        mixed = taps[0:1, :] * padded[pl.ds(9 - n_taps, rows), :]
        for j in range(1, n_taps):
            mixed = mixed + taps[j : j + 1, :] * padded[pl.ds(9 - n_taps + j, rows), :]
        conv[...] = (outer_proj * mixed).astype(BF16)

        loads[7].wait()

        ordered[0:mix_rows, :] = parity_rows(conv, c_no, mix_share, everything)
        ordered[mix_rows:, :] = parity_rows(conv, c_me, mix_share, everything)

        def mix_tile(cols):
            both = jnp.dot(ordered[...], mw[:, cols], preferred_element_type=F32)
            pair_out[:, cols] = both[0:mix_rows].astype(BF16)
            keep[:, cols] = both[mix_rows:]

        column_tiles(width, 512, mix_tile)
        go(pair_copy)

    def mixer_sums():
        pair_copy.wait_recv()

        def sum_tile(cols):
            total = keep[:, cols] + pair_in[:, cols].astype(F32)
            keep[:, cols] = total
            pair_in[:, cols] = total.astype(BF16)

        column_tiles(width, 512, sum_tile)

        for z in z_peers:
            go(
                remote(
                    pair_in.at[z_rows(z, mix_share), :], zin.at[z_me], mz_s.at[z], mz_r.at[z_me],
                    e_me, z * CORES + c_me,
                )
            )

    def forward(q):
        cols = pl.ds(*part_slice(q))
        for e in ep_peers:
            here = got.at[half_rows(c_me, e), cols]
            remote(here, here, disp_s.at[q, e], disp_r.at[q, e], e, t_me).wait_recv()
            go(remote(here, here, fwd_s.at[q, e], fwd_r.at[q, e], e_me, partner))

    def forwarded(q):
        cols = pl.ds(*part_slice(q))
        for e in ep_peers:
            there = got.at[half_rows(c_no, e), cols]
            remote(there, there, fwd_s.at[q, e], fwd_r.at[q, e], e_me, partner).wait_recv()

    arrived_lane = iota((2 * span, 128), 1)

    def project(q):
        first, size = part_slice(q)
        cols = slice(first, first + size)

        def expert(k, carry):
            gate = jnp.dot(got[:, cols], gw[k, cols, :], preferred_element_type=F32)
            up = jnp.dot(got[:, cols], uw[k, cols, :], preferred_element_type=F32)
            if q:
                gate = gate + gate_acc[k]
                up = up + up_acc[k]
            if q < PARTS - 1:
                gate_acc[k] = gate
                up_acc[k] = up
                return carry
            weight = jnp.sum(
                jnp.where(arrived_lane == e_me * experts_here + k, wrow[...], 0.0),
                axis=1, keepdims=True,
            )
            hid[k] = (gate / (1.0 + jnp.exp(-gate)) * up * weight).astype(BF16)
            return carry

        lax.fori_loop(0, experts_here, expert, 0)

    forward(0)
    for k in range(experts_here):
        pltpu.make_async_copy(gate_w.at[k], gw.at[k], gate_sem.at[k]).wait()
        pltpu.make_async_copy(up_w.at[k], uw.at[k], up_sem.at[k]).wait()
    for q in range(PARTS):
        if q + 1 < PARTS:
            forward(q + 1)
            if q == 1:
                mixer_sums()
        else:
            for e in ep_peers:
                remote(wgot.at[e], wgot.at[e], w_s.at[e], w_r.at[e], e, t_me).wait_recv()
            for c in range(CORES):
                for e in range(ep):
                    wrow[c * span + e * half : c * span + (e + 1) * half, :] = wgot[
                        e, c * half : (c + 1) * half, :
                    ]
        forwarded(q)
        project(q)
        if q == 0:
            mixer_pair()
    for k in range(experts_here):
        pltpu.make_async_copy(down_w.at[k], dw.at[k], down_sem.at[k]).wait()

    chunk = width // CHUNKS
    tile = min(512, chunk)

    def core_rows(c):
        return pl.ds(pl.multiple_of(c * span, span), span)

    y_copies = {}

    def stage_a(j):
        for i in range(chunk // tile):
            at = slice(i * tile, (i + 1) * tile)
            cols = slice(j * chunk + i * tile, j * chunk + (i + 1) * tile)
            both = jnp.dot(hid[0], dw[0, :, cols], preferred_element_type=F32)
            for k in range(1, experts_here):
                both = both + jnp.dot(hid[k], dw[k, :, cols], preferred_element_type=F32)
            both_y[...] = both
            y_out[j, :, at] = both_y[core_rows(c_no), :].astype(BF16)
            y_keep[j % 3, :, at] = both_y[core_rows(c_me), :]
        y_copies[j] = remote(y_out.at[j], y_in.at[j], yp_s.at[j], yp_r.at[j], e_me, partner)
        go(y_copies[j])

    def e_rows(e):
        return pl.ds(pl.multiple_of(e * half, half), half)

    def stage_b(j):
        y_copies[j].wait_recv()
        y_in[j] = (y_keep[j % 3] + y_in[j].astype(F32)).astype(BF16)
        for e in ep_peers:
            go(
                remote(
                    y_in.at[j, e_rows(e), :], e_in.at[j, e_rows(e_me), :],
                    ye_s.at[j, e], ye_r.at[j, e_me], e, t_me,
                )
            )
        e_in[j, e_rows(e_me), :] = y_in[j, e_rows(e_me), :]

    def stage_c(j):
        for e in ep_peers:
            here = e_in.at[j, e_rows(e), :]
            remote(here, here, ye_s.at[j, e], ye_r.at[j, e], e, t_me).wait_recv()
        own = parity_rows(spread, c_me, share, core_rows(c_me))
        total = jnp.dot(own, e_in[j], preferred_element_type=F32)
        s_out[j] = total.astype(BF16)
        for z in z_peers:
            go(
                remote(
                    s_out.at[j, z_rows(z, share), :], s_in.at[j, z_me],
                    yz_s.at[j, z], yz_r.at[j, z_me], e_me, z * CORES + c_me,
                )
            )
        s_keep[j % 4] = total

    def stage_d(j):
        total = s_keep[j % 4, z_rows(z_me, share), :]
        for z in z_peers:
            here = s_in.at[j, z]
            remote(here, here, yz_s.at[j, z], yz_r.at[j, z], e_me, z * CORES + c_me).wait_recv()
            total = total + s_in[j, z].astype(F32)
        expert_out[:, j * chunk : (j + 1) * chunk] = total.astype(BF16)

    def mixer_final():
        total = keep[z_rows(z_me, mix_share), :]
        for z in z_peers:
            here = zin.at[z]
            remote(here, here, mz_s.at[z], mz_r.at[z], e_me, z * CORES + c_me).wait_recv()
            total = total + zin[z].astype(F32)
        mixer_out[...] = total.astype(BF16)

    lag_b, lag_c, lag_d = 2, 7, 10
    for step in range(CHUNKS + lag_d):
        for stage, lag in ((stage_a, 0), (stage_b, lag_b), (stage_c, lag_c), (stage_d, lag_d)):
            if 0 <= step - lag < CHUNKS:
                stage(step - lag)
        if step == CHUNKS:
            mixer_final()

    for copy in sends:
        copy.wait_send()


def store(a, b, a_out, b_out, held, sem):
    refs = ((a, a_out), (b, b_out))
    into = [pltpu.make_async_copy(s, held.at[i], sem.at[0, i]) for i, (s, _) in enumerate(refs)]
    outof = [pltpu.make_async_copy(held.at[i], d, sem.at[1, i]) for i, (_, d) in enumerate(refs)]
    for c in into:
        c.start()
    for c, d in zip(into, outof):
        c.wait()
        d.start()
    for d in outof:
        d.wait()


def local(ep, tp, *args):
    (mix_tokens, mix_gain, value_w, inner_w, outer_w, taps, mix_w, moe_tokens, moe_gain,
     router_group, router_expert, routes, gate_w, up_w, down_w) = args
    rows, width = mix_tokens.shape
    count = moe_tokens.shape[0]
    channels, hidden = value_w.shape[1], gate_w.shape[2]
    experts_here = gate_w.shape[0]
    zs = tp // CORES
    share, mix_share = count // tp, rows // tp
    topk = routes.shape[1]
    slots = experts_here * CAP
    if experts_here % EPG == 0:
        slots = slots // topk
    slots = min(slots, share)
    half = zs * slots
    span = ep * half
    chunk = width // CHUNKS
    any_ref = pl.BlockSpec(memory_space=pl.ANY)
    vmem = pl.BlockSpec(memory_space=pltpu.VMEM)
    V, D = pltpu.VMEM, lambda *s: pltpu.SemaphoreType.DMA(s)
    scratch = [
        V((rows, width), BF16), V((count, width), BF16),
        V(router_group.T.shape, BF16), V(router_expert.T.shape, BF16),
        V(value_w.shape, BF16), V(inner_w.shape, BF16), V(outer_w.shape, BF16),
        V(mix_w.shape, BF16),
        V(gate_w.shape, BF16), V(up_w.shape, BF16), V(down_w.shape, BF16),
        V((rows, width), BF16), V((count, width), BF16), V((count, 2 * span), BF16), V((2 * span, count), BF16),
        V((2 * span, width), BF16), V((2 * span, width), BF16),
        V((ep, 2 * half, 128), F32), V((ep, 2 * half, 128), F32), V((2 * span, 128), F32),
        V((rows, channels), BF16), V((16, channels), BF16), V((rows + 8, channels), F32),
        V((rows, channels), BF16), V((rows, channels), BF16),
        V((zs * mix_share, width), BF16), V((zs * mix_share, width), BF16),
        V((zs * mix_share, width), F32),
        V((zs, mix_share, width), BF16),
        V((experts_here, 2 * span, hidden), F32), V((experts_here, 2 * span, hidden), F32),
        V((experts_here, 2 * span, hidden), BF16), V((2 * span, min(512, chunk)), F32),
        V((CHUNKS, span, chunk), BF16), V((CHUNKS, span, chunk), BF16),
        V((3, span, chunk), F32),
        V((CHUNKS, span, chunk), BF16),
        V((4, zs * share, chunk), F32), V((CHUNKS, zs * share, chunk), BF16),
        V((CHUNKS, zs, share, chunk), BF16),
        D(8), D(experts_here), D(experts_here), D(experts_here),
        D(PARTS, ep), D(PARTS, ep), D(ep), D(ep), D(PARTS, ep), D(PARTS, ep), D(1), D(1), D(1), D(1), D(zs), D(zs),
        D(CHUNKS), D(CHUNKS), D(CHUNKS, ep), D(CHUNKS, ep), D(CHUNKS, zs), D(CHUNKS, zs),
    ]
    out = [
        jax.ShapeDtypeStruct((mix_share, width), BF16),
        jax.ShapeDtypeStruct((share, width), BF16),
    ]
    in_specs = [
        any_ref, vmem, any_ref, any_ref, any_ref, vmem, any_ref, any_ref, vmem,
        any_ref, any_ref, vmem, any_ref, any_ref, any_ref,
    ]
    results = pl.pallas_call(
        functools.partial(kernel, (ep, tp, zs, half, experts_here)),
        out_shape=out,
        in_specs=in_specs,
        out_specs=[vmem, vmem],
        scratch_shapes=scratch,
        compiler_params=pltpu.CompilerParams(
            collective_id=0, has_side_effects=True, vmem_limit_bytes=67043328
        ),
        name="mixer_and_experts",
    )(
        mix_tokens, mix_gain.reshape(1, width), value_w, inner_w, outer_w, taps, mix_w,
        moe_tokens, moe_gain.reshape(1, width), router_group.T, router_expert.T, routes.T,
        gate_w, up_w, down_w,
    )
    return pl.pallas_call(
        store,
        out_shape=out,
        in_specs=[any_ref, any_ref],
        out_specs=[any_ref, any_ref],
        scratch_shapes=[V((2, share, width), BF16), D(2, 2)],
        name="store",
    )(*results)


def solution(mesh):
    return jax.shard_map(
        lambda *args: tuple(local(mesh.shape["ep"], mesh.shape["tp"], *args)),
        mesh=mesh,
        in_specs=(
            P("ep", None), P(), P(None, "tp"), P(None, "tp"), P(None, "tp"), P(None, "tp"),
            P("tp", None), P("ep", None), P(), P(), P(), P("ep", None),
            P("ep", None, "tp"), P("ep", None, "tp"), P("ep", "tp", None),
        ),
        out_specs=(P(("ep", "tp"), None), P(("ep", "tp"), None)),
        check_vma=False,
    )
```

```python
import functools

import jax
import jax.numpy as jnp
from jax import lax
from jax.experimental import pallas as pl
from jax.experimental.pallas import tpu as pltpu
from jax.sharding import PartitionSpec as P

EPG = 4
CAP = 4
CORES = 2
CHUNKS = 8
SPLIT = (2, 2, 3, 1)
PARTS = len(SPLIT)
MESH = pl.DeviceIdType.MESH
F32, BF16 = jnp.float32, jnp.bfloat16


def iota(shape, dim):
    return lax.broadcasted_iota(jnp.int32, shape, dim)


def norm_rows(src, gain, dst):
    width = src.shape[1]

    def body(i, carry):
        rows = pl.ds(pl.multiple_of(i * 16, 16), 16)
        x = src[rows, :].astype(F32)
        inv = lax.rsqrt(jnp.sum(x * x, axis=1, keepdims=True) * (1.0 / width) + 1e-06)
        dst[rows, :] = (x * inv * gain[...]).astype(BF16)
        return carry

    lax.fori_loop(0, src.shape[0] // 16, body, 0)


def column_tiles(width, tile, body):
    def step(i, carry):
        body(pl.ds(pl.multiple_of(i * tile, tile), tile))
        return carry

    lax.fori_loop(0, width // tile, step, 0)


def kernel(
    cfg,
    mix_tokens, mix_gain, value_w, inner_w, outer_w, taps, mix_w, moe_tokens, moe_gain,
    router_group, router_expert, routes, gate_w, up_w, down_w,
    mixer_out, expert_out,
    xm, xe, rg, rx, vw, iw, ow, mw, gw, uw, dw,
    nm, ne, spread, gather, pack, got, wpack, wgot, wrow,
    gated, halo, padded, conv, ordered, pair_out, pair_in, keep, zin,
    gate_acc, up_acc, hid, both_y, y_out, y_in, y_keep, e_in, s_keep, s_out, s_in,
    load_sem, gate_sem, up_sem, down_sem,
    disp_s, disp_r, w_s, w_r, fwd_s, fwd_r, halo_s, halo_r, mp_s, mp_r, mz_s, mz_r,
    yp_s, yp_r, ye_s, ye_r, yz_s, yz_r,
):
    ep, tp, zs, half, experts_here = cfg
    e_me, t_me = lax.axis_index("ep"), lax.axis_index("tp")
    z_me, c_me = t_me // CORES, lax.rem(t_me, CORES)
    c_no = 1 - c_me
    partner = z_me * CORES + c_no
    width = xm.shape[1]
    ep_peers = [lax.rem(e_me + d, ep) for d in range(1, ep)]
    z_peers = [lax.rem(z_me + d, zs) for d in range(1, zs)]

    barrier = pltpu.get_barrier_semaphore()
    for e in ep_peers:
        pl.semaphore_signal(barrier, inc=1, device_id={"ep": e, "tp": t_me}, device_id_type=MESH)
    for z in z_peers:
        pl.semaphore_signal(
            barrier, inc=1, device_id={"ep": e_me, "tp": z * CORES + c_me}, device_id_type=MESH
        )
    pl.semaphore_signal(barrier, inc=1, device_id={"ep": e_me, "tp": partner}, device_id_type=MESH)

    def load(k, src, dst):
        return pltpu.make_async_copy(src, dst, load_sem.at[k])

    loads = [
        load(k, s, d)
        for k, (s, d) in enumerate(
            [
                (moe_tokens, xe), (router_group, rg), (router_expert, rx), (mix_tokens, xm),
                (value_w, vw), (inner_w, iw), (outer_w, ow), (mix_w, mw),
            ]
        )
    ]
    for c in loads:
        c.start()

    def remote(src, dst, s_sem, r_sem, e, t):
        return pltpu.make_async_remote_copy(
            src_ref=src, dst_ref=dst, send_sem=s_sem, recv_sem=r_sem,
            device_id={"ep": e, "tp": t}, device_id_type=MESH,
        )

    count = xe.shape[0]
    share = count // tp
    slots = half // zs
    span = ep * half
    diagonal = jnp.where(iota((count, count), 0) == iota((count, count), 1), 1.0, 0.0)
    r = lax.dot_general(
        diagonal.astype(BF16), routes[...].astype(F32).astype(BF16), (((1,), (1,)), ((), ())),
        preferred_element_type=F32,
    ).astype(jnp.int32)
    picks = [r[:, 0:1], r[:, 1:2]]
    lane = iota((count, 128), 1)
    shards = [
        sum((p >= s * experts_here).astype(jnp.int32) for s in range(1, ep)) for p in picks
    ]
    member = jnp.where((lane == shards[0]) | (lane == shards[1]), 1.0, 0.0).astype(BF16)
    ti, tj = iota((count, count), 0), iota((count, count), 1)
    earlier = jnp.where(((ti ^ tj) < share) & (tj < ti), 1.0, 0.0).astype(BF16)
    rank = jnp.dot(earlier, member, preferred_element_type=F32)
    block = lax.shift_right_logical(iota((count, 1), 0), share.bit_length() - 1)
    base = (block & 1) * span + lax.shift_right_logical(block, 1) * slots
    slot_lane = iota((count, 2 * span), 1)
    hits = []
    for s in shards:
        mine = jnp.sum(jnp.where(lane == s, rank, 0.0), axis=1, keepdims=True).astype(jnp.int32)
        hits.append(slot_lane == base + s * half + mine)
    one_hot = jnp.where(hits[0] | hits[1], 1.0, 0.0).astype(BF16)
    spread[...] = one_hot
    gather[...] = lax.dot_general(
        one_hot, diagonal.astype(BF16), (((0,), (0,)), ((), ())), preferred_element_type=F32
    ).astype(BF16)
    loads[0].wait()
    for k in range(experts_here):
        pltpu.make_async_copy(gate_w.at[k], gw.at[k], gate_sem.at[k]).start()
        pltpu.make_async_copy(up_w.at[k], uw.at[k], up_sem.at[k]).start()
    for k in range(experts_here):
        pltpu.make_async_copy(down_w.at[k], dw.at[k], down_sem.at[k]).start()
    norm_rows(xe, moe_gain, ne)
    unit = width // sum(SPLIT)

    def part_slice(q):
        return sum(SPLIT[:q]) * unit, SPLIT[q] * unit

    def pack_part(q):
        first, size = part_slice(q)
        cols = slice(first, first + size)
        pack[:, cols] = jnp.dot(
            gather[...], ne[:, cols], preferred_element_type=F32
        ).astype(BF16)

    pack_part(0)
    pl.semaphore_wait(barrier, (ep - 1) + (zs - 1) + 1)
    sends = []

    def go(copy):
        copy.start()
        sends.append(copy)

    def half_rows(c, e):
        return pl.ds(pl.multiple_of(c * span + e * half, half), half)

    def dispatch(q):
        cols = pl.ds(*part_slice(q))
        for e in ep_peers:
            go(
                remote(
                    pack.at[half_rows(c_me, e), cols], got.at[half_rows(c_me, e_me), cols],
                    disp_s.at[q, e], disp_r.at[q, e_me], e, t_me,
                )
            )

    early = PARTS // 2
    for q in range(1, PARTS):
        if q <= early:
            dispatch(q - 1)
        pack_part(q)
    loads[1].wait()
    loads[2].wait()
    lanes = (((1,), (1,)), ((), ()))
    group_exp = jnp.exp(lax.dot_general(ne[...], rg[...], lanes, preferred_element_type=F32))
    expert_logit = lax.dot_general(ne[...], rx[...], lanes, preferred_element_type=F32)
    groups, experts = group_exp.shape[1], expert_logit.shape[1]
    group = sum((picks[0] >= s * EPG).astype(jnp.int32) for s in range(1, groups))
    chosen_group = jnp.where(iota((count, groups), 1) == group, group_exp, 0.0)
    group_gate = jnp.sum(chosen_group, axis=1, keepdims=True) / jnp.sum(
        group_exp, axis=1, keepdims=True
    )
    expert_lane = iota((count, experts), 1)
    chosen = [
        jnp.exp(jnp.sum(jnp.where(expert_lane == p, expert_logit, 0.0), axis=1, keepdims=True))
        for p in picks
    ]
    scale = chosen[0] + chosen[1]
    weights = sum(
        jnp.where(lane == p, group_gate * c / scale, 0.0) for p, c in zip(picks, chosen)
    )
    parts, rest = [], weights
    for _ in range(3):
        parts.append(rest.astype(BF16))
        rest = rest - parts[-1].astype(F32)
    packed_w = sum(jnp.dot(gather[...], p, preferred_element_type=F32) for p in parts)
    for e in range(ep):
        for c in range(CORES):
            wpack[e, c * half : (c + 1) * half, :] = packed_w[
                c * span + e * half : c * span + (e + 1) * half, :
            ]
    wgot[e_me] = wpack[e_me]
    for c in range(CORES):
        got[half_rows(c, e_me), :] = pack[half_rows(c, e_me), :]

    loads[3].wait()
    norm_rows(xm, mix_gain, nm)
    loads[4].wait()
    loads[5].wait()
    rows = xm.shape[0]
    value_proj = jnp.dot(nm[...], vw[...], preferred_element_type=F32)
    inner_proj = jnp.dot(nm[...], iw[...], preferred_element_type=F32)
    gated[...] = (inner_proj * value_proj).astype(BF16)
    halo_copy = remote(
        gated.at[pl.ds(rows - 16, 16), :], halo, halo_s.at[0], halo_r.at[0],
        lax.rem(e_me + 1, ep), t_me,
    )
    halo_copy.start()
    for q in range(early, PARTS):
        dispatch(q)
        if q == early:
            for e in ep_peers:
                go(remote(wpack.at[e], wgot.at[e_me], w_s.at[e], w_r.at[e_me], e, t_me))
    padded[8:, :] = gated[...].astype(F32)
    loads[6].wait()
    outer_proj = jnp.dot(nm[...], ow[...], preferred_element_type=F32)
    mix_share = rows // tp
    mix_rows = zs * mix_share
    everything = slice(None)
    pair_copy = remote(pair_out, pair_in, mp_s.at[0], mp_r.at[0], e_me, partner)

    def parity_rows(ref, c, step, cols):
        return jnp.concatenate(
            [
                ref[pl.ds(pl.multiple_of((z * CORES + c) * step, step), step), cols]
                for z in range(zs)
            ],
            axis=0,
        )

    def z_rows(z, step):
        return pl.ds(pl.multiple_of(z * step, step), step)

    def mixer_pair():
        halo_copy.wait()
        before = halo[...].astype(F32)[8:16, :]
        padded[0:8, :] = jnp.where(e_me > 0, before, jnp.zeros_like(before))
        n_taps = taps.shape[0]
        mixed = taps[0:1, :] * padded[pl.ds(9 - n_taps, rows), :]
        for j in range(1, n_taps):
            mixed = mixed + taps[j : j + 1, :] * padded[pl.ds(9 - n_taps + j, rows), :]
        conv[...] = (outer_proj * mixed).astype(BF16)

        loads[7].wait()

        ordered[0:mix_rows, :] = parity_rows(conv, c_no, mix_share, everything)
        ordered[mix_rows:, :] = parity_rows(conv, c_me, mix_share, everything)

        def mix_tile(cols):
            both = jnp.dot(ordered[...], mw[:, cols], preferred_element_type=F32)
            pair_out[:, cols] = both[0:mix_rows].astype(BF16)
            keep[:, cols] = both[mix_rows:]

        column_tiles(width, 512, mix_tile)
        go(pair_copy)

    def mixer_sums():
        pair_copy.wait_recv()

        def sum_tile(cols):
            total = keep[:, cols] + pair_in[:, cols].astype(F32)
            keep[:, cols] = total
            pair_in[:, cols] = total.astype(BF16)

        column_tiles(width, 512, sum_tile)

        for z in z_peers:
            go(
                remote(
                    pair_in.at[z_rows(z, mix_share), :], zin.at[z_me], mz_s.at[z], mz_r.at[z_me],
                    e_me, z * CORES + c_me,
                )
            )

    def forward(q):
        cols = pl.ds(*part_slice(q))
        for e in ep_peers:
            here = got.at[half_rows(c_me, e), cols]
            remote(here, here, disp_s.at[q, e], disp_r.at[q, e], e, t_me).wait_recv()
            go(remote(here, here, fwd_s.at[q, e], fwd_r.at[q, e], e_me, partner))

    def forwarded(q):
        cols = pl.ds(*part_slice(q))
        for e in ep_peers:
            there = got.at[half_rows(c_no, e), cols]
            remote(there, there, fwd_s.at[q, e], fwd_r.at[q, e], e_me, partner).wait_recv()

    arrived_lane = iota((2 * span, 128), 1)

    def project(q):
        first, size = part_slice(q)
        cols = slice(first, first + size)

        def expert(k, carry):
            gate = jnp.dot(got[:, cols], gw[k, cols, :], preferred_element_type=F32)
            up = jnp.dot(got[:, cols], uw[k, cols, :], preferred_element_type=F32)
            if q:
                gate = gate + gate_acc[k]
                up = up + up_acc[k]
            if q < PARTS - 1:
                gate_acc[k] = gate
                up_acc[k] = up
                return carry
            weight = jnp.sum(
                jnp.where(arrived_lane == e_me * experts_here + k, wrow[...], 0.0),
                axis=1, keepdims=True,
            )
            hid[k] = (gate / (1.0 + jnp.exp(-gate)) * up * weight).astype(BF16)
            return carry

        lax.fori_loop(0, experts_here, expert, 0)

    forward(0)
    for k in range(experts_here):
        pltpu.make_async_copy(gate_w.at[k], gw.at[k], gate_sem.at[k]).wait()
        pltpu.make_async_copy(up_w.at[k], uw.at[k], up_sem.at[k]).wait()
    for q in range(PARTS):
        if q + 1 < PARTS:
            forward(q + 1)
            if q == 1:
                mixer_sums()
        else:
            for e in ep_peers:
                remote(wgot.at[e], wgot.at[e], w_s.at[e], w_r.at[e], e, t_me).wait_recv()
            for c in range(CORES):
                for e in range(ep):
                    wrow[c * span + e * half : c * span + (e + 1) * half, :] = wgot[
                        e, c * half : (c + 1) * half, :
                    ]
        forwarded(q)
        project(q)
        if q == 0:
            mixer_pair()
    for k in range(experts_here):
        pltpu.make_async_copy(down_w.at[k], dw.at[k], down_sem.at[k]).wait()

    chunk = width // CHUNKS
    tile = min(512, chunk)

    def core_rows(c):
        return pl.ds(pl.multiple_of(c * span, span), span)

    y_copies = {}

    def stage_a(j):
        for i in range(chunk // tile):
            at = slice(i * tile, (i + 1) * tile)
            cols = slice(j * chunk + i * tile, j * chunk + (i + 1) * tile)
            both = jnp.dot(hid[0], dw[0, :, cols], preferred_element_type=F32)
            for k in range(1, experts_here):
                both = both + jnp.dot(hid[k], dw[k, :, cols], preferred_element_type=F32)
            both_y[...] = both
            y_out[j, :, at] = both_y[core_rows(c_no), :].astype(BF16)
            y_keep[j % 3, :, at] = both_y[core_rows(c_me), :]
        y_copies[j] = remote(y_out.at[j], y_in.at[j], yp_s.at[j], yp_r.at[j], e_me, partner)
        go(y_copies[j])

    def e_rows(e):
        return pl.ds(pl.multiple_of(e * half, half), half)

    def stage_b(j):
        y_copies[j].wait_recv()
        y_in[j] = (y_keep[j % 3] + y_in[j].astype(F32)).astype(BF16)
        for e in ep_peers:
            go(
                remote(
                    y_in.at[j, e_rows(e), :], e_in.at[j, e_rows(e_me), :],
                    ye_s.at[j, e], ye_r.at[j, e_me], e, t_me,
                )
            )
        e_in[j, e_rows(e_me), :] = y_in[j, e_rows(e_me), :]

    def stage_c(j):
        for e in ep_peers:
            here = e_in.at[j, e_rows(e), :]
            remote(here, here, ye_s.at[j, e], ye_r.at[j, e], e, t_me).wait_recv()
        own = parity_rows(spread, c_me, share, core_rows(c_me))
        total = jnp.dot(own, e_in[j], preferred_element_type=F32)
        s_out[j] = total.astype(BF16)
        for z in z_peers:
            go(
                remote(
                    s_out.at[j, z_rows(z, share), :], s_in.at[j, z_me],
                    yz_s.at[j, z], yz_r.at[j, z_me], e_me, z * CORES + c_me,
                )
            )
        s_keep[j % 4] = total

    def stage_d(j):
        total = s_keep[j % 4, z_rows(z_me, share), :]
        for z in z_peers:
            here = s_in.at[j, z]
            remote(here, here, yz_s.at[j, z], yz_r.at[j, z], e_me, z * CORES + c_me).wait_recv()
            total = total + s_in[j, z].astype(F32)
        expert_out[:, j * chunk : (j + 1) * chunk] = total.astype(BF16)

    def mixer_final():
        total = keep[z_rows(z_me, mix_share), :]
        for z in z_peers:
            here = zin.at[z]
            remote(here, here, mz_s.at[z], mz_r.at[z], e_me, z * CORES + c_me).wait_recv()
            total = total + zin[z].astype(F32)
        mixer_out[...] = total.astype(BF16)

    lag_b, lag_c, lag_d = 2, 7, 10
    for step in range(CHUNKS + lag_d):
        for stage, lag in ((stage_a, 0), (stage_b, lag_b), (stage_c, lag_c), (stage_d, lag_d)):
            if 0 <= step - lag < CHUNKS:
                stage(step - lag)
        if step == CHUNKS:
            mixer_final()

    for copy in sends:
        copy.wait_send()


def store(a, b, a_out, b_out, held, sem):
    refs = ((a, a_out), (b, b_out))
    into = [pltpu.make_async_copy(s, held.at[i], sem.at[0, i]) for i, (s, _) in enumerate(refs)]
    outof = [pltpu.make_async_copy(held.at[i], d, sem.at[1, i]) for i, (_, d) in enumerate(refs)]
    for c in into:
        c.start()
    for c, d in zip(into, outof):
        c.wait()
        d.start()
    for d in outof:
        d.wait()


def local(ep, tp, *args):
    (mix_tokens, mix_gain, value_w, inner_w, outer_w, taps, mix_w, moe_tokens, moe_gain,
     router_group, router_expert, routes, gate_w, up_w, down_w) = args
    rows, width = mix_tokens.shape
    count = moe_tokens.shape[0]
    channels, hidden = value_w.shape[1], gate_w.shape[2]
    experts_here = gate_w.shape[0]
    zs = tp // CORES
    share, mix_share = count // tp, rows // tp
    topk = routes.shape[1]
    slots = experts_here * CAP
    if experts_here % EPG == 0:
        slots = slots // topk
    slots = min(slots, share)
    half = zs * slots
    span = ep * half
    chunk = width // CHUNKS
    any_ref = pl.BlockSpec(memory_space=pl.ANY)
    vmem = pl.BlockSpec(memory_space=pltpu.VMEM)
    V, D = pltpu.VMEM, lambda *s: pltpu.SemaphoreType.DMA(s)
    scratch = [
        V((rows, width), BF16), V((count, width), BF16),
        V(router_group.T.shape, BF16), V(router_expert.T.shape, BF16),
        V(value_w.shape, BF16), V(inner_w.shape, BF16), V(outer_w.shape, BF16),
        V(mix_w.shape, BF16),
        V(gate_w.shape, BF16), V(up_w.shape, BF16), V(down_w.shape, BF16),
        V((rows, width), BF16), V((count, width), BF16), V((count, 2 * span), BF16), V((2 * span, count), BF16),
        V((2 * span, width), BF16), V((2 * span, width), BF16),
        V((ep, 2 * half, 128), F32), V((ep, 2 * half, 128), F32), V((2 * span, 128), F32),
        V((rows, channels), BF16), V((16, channels), BF16), V((rows + 8, channels), F32),
        V((rows, channels), BF16), V((rows, channels), BF16),
        V((zs * mix_share, width), BF16), V((zs * mix_share, width), BF16),
        V((zs * mix_share, width), F32),
        V((zs, mix_share, width), BF16),
        V((experts_here, 2 * span, hidden), F32), V((experts_here, 2 * span, hidden), F32),
        V((experts_here, 2 * span, hidden), BF16), V((2 * span, min(512, chunk)), F32),
        V((CHUNKS, span, chunk), BF16), V((CHUNKS, span, chunk), BF16),
        V((3, span, chunk), F32),
        V((CHUNKS, span, chunk), BF16),
        V((4, zs * share, chunk), F32), V((CHUNKS, zs * share, chunk), BF16),
        V((CHUNKS, zs, share, chunk), BF16),
        D(8), D(experts_here), D(experts_here), D(experts_here),
        D(PARTS, ep), D(PARTS, ep), D(ep), D(ep), D(PARTS, ep), D(PARTS, ep), D(1), D(1), D(1), D(1), D(zs), D(zs),
        D(CHUNKS), D(CHUNKS), D(CHUNKS, ep), D(CHUNKS, ep), D(CHUNKS, zs), D(CHUNKS, zs),
    ]
    out = [
        jax.ShapeDtypeStruct((mix_share, width), BF16),
        jax.ShapeDtypeStruct((share, width), BF16),
    ]
    in_specs = [
        any_ref, vmem, any_ref, any_ref, any_ref, vmem, any_ref, any_ref, vmem,
        any_ref, any_ref, vmem, any_ref, any_ref, any_ref,
    ]
    results = pl.pallas_call(
        functools.partial(kernel, (ep, tp, zs, half, experts_here)),
        out_shape=out,
        in_specs=in_specs,
        out_specs=[vmem, vmem],
        scratch_shapes=scratch,
        compiler_params=pltpu.CompilerParams(
            collective_id=0, has_side_effects=True, vmem_limit_bytes=67043328
        ),
        name="mixer_and_experts",
    )(
        mix_tokens, mix_gain.reshape(1, width), value_w, inner_w, outer_w, taps, mix_w,
        moe_tokens, moe_gain.reshape(1, width), router_group.T, router_expert.T, routes.T,
        gate_w, up_w, down_w,
    )
    return pl.pallas_call(
        store,
        out_shape=out,
        in_specs=[any_ref, any_ref],
        out_specs=[any_ref, any_ref],
        scratch_shapes=[V((2, share, width), BF16), D(2, 2)],
        name="store",
    )(*results)


def solution(mesh):
    return jax.shard_map(
        lambda *args: tuple(local(mesh.shape["ep"], mesh.shape["tp"], *args)),
        mesh=mesh,
        in_specs=(
            P("ep", None), P(), P(None, "tp"), P(None, "tp"), P(None, "tp"), P(None, "tp"),
            P("tp", None), P("ep", None), P(), P(), P(), P("ep", None),
            P("ep", None, "tp"), P("ep", None, "tp"), P("ep", "tp", None),
        ),
        out_specs=(P(("ep", "tp"), None), P(("ep", "tp"), None)),
        check_vma=False,
    )
```
